256 devices in a mesh: ep: 16 (over y, x), tp: 16 (over z, core).
Axes of the slice: x: 4, y: 4, z: 8, core: 2. Of those that a mesh axis runs over, the one named last changes fastest.
Arguments:
- q_latent: bfloat16 [16384, 512], P('ep'), may hold values from -6 to 6
- kv_latent: bfloat16 [16384, 256], P('ep'), may hold values from -6 to 6
- rope_key: bfloat16 [16384, 32], P('ep'), may hold values from -1200 to 1200
- q_gain: float32 [512], replicated, may hold values from 0.1 to 1.9
- kv_gain: float32 [256], replicated, may hold values from 0.1 to 1.9
- w_query: bfloat16 [512, 1536], P(None, 'tp'), may hold values from -0.25 to 0.25
- w_keyval: bfloat16 [256, 2048], P(None, 'tp'), may hold values from -0.375 to 0.375
- w_output: bfloat16 [1024, 2048], P(None, 'tp'), may hold values from -0.1875 to 0.1875
- moe_input: bfloat16 [8192, 2048], P('ep'), may hold values from -6 to 6
- moe_gain: float32 [2048], replicated, may hold values from 0.1 to 1.9
- routes: int32 [8192, 2], P('ep'), may hold values from 0 to 15, all different within a row; in each aligned block of 32 rows (0 to 31, 32 to 63, ...) at most 6 rows name the same one
- route_weight: float32 [8192, 2], P('ep'), may hold values from 0.25 to 2
- expert_gate: bfloat16 [16, 2048, 4096], P('ep', None, 'tp'), may hold values from -0.125 to 0.125
- expert_up: bfloat16 [16, 2048, 4096], P('ep', None, 'tp'), may hold values from -0.125 to 0.125
- expert_down: bfloat16 [16, 4096, 2048], P('ep', 'tp'), may hold values from -0.09375 to 0.09375
- shared_gate: bfloat16 [2048, 2048], P(None, 'tp'), may hold values from -0.125 to 0.125
- shared_up: bfloat16 [2048, 2048], P(None, 'tp'), may hold values from -0.125 to 0.125
- shared_down: bfloat16 [2048, 2048], P('tp'), may hold values from -0.125 to 0.125
Outputs:
- mixed: bfloat16 [16384, 2048], P('ep', 'tp')
- moe_out: bfloat16 [8192, 2048], P(('ep', 'tp'))
The draws below stay inside these ranges and needn't reach their ends.
Inputs may be any that keep to these rules, and one draw needn't show every extreme that they name: `routes`: in each aligned block of 32 rows (the rows of one device's output) no expert is named by more than 6 rows, a bound that some block reaches. Each row names 2 different experts.
All inputs are finite; a program needn't handle non-finite values.
Results may differ from the reference program's by a relative error of at most 0.023.
Values may be sent and summed in bfloat16 or wider, within the bound.
No kernel may reach another device: no remote copies, remote signals or barrier semaphores. Data moves between devices by JAX's collectives and lax.ppermute only.
A program may use at most 128 MiB of HBM per device.

```python
import math
import jax
import jax.numpy as jnp
import numpy as np
from jax import lax

D = 2048
HEADS = 16
NOPE = 64
ROPE_DIM = 32
VDIM = 64
QLAT = 512
KVLAT = 256
TOKA_EP = 1024
TOK_A = 16384
MOE_DEV = 32
TOK_B = 8192
EXPERTS = 16
FE = 4096
FS = 2048
FE_PART = 256
FS_PART = 128
TOP = 2
CAP = 6
N_EP = 16
N_TP = 16


def draw_rope_key(key, part):
    drawn = jax.random.normal(jax.random.fold_in(key, 11), (TOK_A, ROPE_DIM), jnp.float32)
    drawn = jnp.clip(drawn, -6.0, 6.0)
    return drawn.astype(jnp.bfloat16)


def block_scale(own_key, extent, split, smallest, top_value):
    level = 1.0
    for axis_at, parts in split:
        heights = jax.random.uniform(jax.random.fold_in(jax.random.fold_in(own_key, 6), axis_at), (parts,), jnp.float32, smallest / len(split), top_value / len(split))
        level = level * jnp.repeat(jnp.exp(heights), extent[axis_at] // parts).reshape((-1,) + (1,) * (len(extent) - 1 - axis_at))
    return level


def routed_block(own_key, own, number, rows, amount, top, bound, skew):
    order = jax.random.permutation(own_key, amount)
    packed, ordinary = shares(amount, rows * top, bound, skew, True), shares(amount, rows * top, bound, skew, False)
    places = jnp.arange(amount)

    def named(lengths, offset_by):
        used = int((lengths > 0).sum())
        fixed = max(1, used // 4)
        passed = fixed + (places - fixed + offset_by * (used - fixed)) % max(1, amount - fixed)
        return jnp.zeros((amount,), jnp.int32).at[order[jnp.where(places < fixed, places, passed)]].set(jnp.asarray(lengths, jnp.int32))

    lengths = jnp.where(number % 4 == 0, named(packed, number // 4), named(ordinary, number - number // 4 - 1))
    mixed = jax.random.permutation(jax.random.fold_in(own, 3), amount)
    source_of, taker = mixed[0:amount // 2 * 2:2], mixed[1:amount // 2 * 2:2]
    room = jnp.minimum(lengths[source_of] - 1, bound - lengths[taker]) // 2
    room = jnp.where((source_of == order[0]) | (taker == order[0]) | (lengths[taker] == 0), 0, jnp.maximum(room, 0))
    passed = jax.random.randint(jax.random.fold_in(own, 4), (amount // 2,), 0, 1 << 20) % (room + 1)
    lengths = lengths.at[source_of].add(-passed).at[taker].add(passed)
    members = jnp.searchsorted(jnp.cumsum(lengths), jnp.arange(rows * top), side="right").astype(jnp.int32)
    grid = members.reshape(top, rows).T
    grid = grid[jax.random.permutation(jax.random.fold_in(own, 1), rows)]
    offset_by = jax.random.randint(jax.random.fold_in(own, 2), (rows, 1), 0, top)
    return jnp.take_along_axis(grid, (jnp.arange(top)[None, :] + offset_by) % top, axis=1)


def shares(amount, total, bound, slope, full):
    portions = [(1 << 20) // math.isqrt(rank ** slope) + 1 for rank in range(1, amount + 1)]
    largest = bound if full else min(bound, max(-(-total // amount), total * portions[0] // sum(portions)))
    least = 1 if total - largest >= amount - 1 else 0
    holding, rest = [largest] + [least] * (amount - 1), total - largest - least * (amount - 1)
    while rest > 0:
        free = [i for i in range(1, amount) if holding[i] < largest] or [i for i in range(1, amount) if holding[i] < bound]
        whole, left = sum([portions[i] for i in free]), rest
        for i in free:
            extra = min(bound - holding[i], max(1, left * portions[i] // whole), rest)
            holding[i] = holding[i] + extra
            rest = rest - extra
    return np.array(holding)


def bell_draw(key, shape, deviation, bound, pieces=(), held_as=jnp.bfloat16):
    values = jax.random.normal(key, shape, jnp.float32) * deviation
    if len(pieces) > 0:
        values = block_scale(key, shape, pieces, -0.22, 0.18) * values
    return jnp.clip(values, min=-bound, max=bound).astype(held_as)


def setup_inputs(seed: int = 0) -> dict:
    streams_of = jax.random.split(jax.random.key(seed), 19)
    q_latent = bell_draw(streams_of[0], (TOK_A, QLAT), 1.0, 6.0, ((0, 16),))
    kv_latent = bell_draw(streams_of[1], (TOK_A, KVLAT), 1.0, 6.0, ((0, 16),))
    rope_key = draw_rope_key(jax.random.fold_in(streams_of[18], 71), 0)
    q_gain = jnp.clip(1.0 + 0.18 * jax.random.normal(streams_of[3], (QLAT,), jnp.float32), 0.1, 1.9)
    kv_gain = jnp.clip(1.0 + 0.18 * jax.random.normal(streams_of[4], (KVLAT,), jnp.float32), 0.1, 1.9)
    w_query = bell_draw(streams_of[5], (QLAT, HEADS * (NOPE + ROPE_DIM)), QLAT ** -0.5, 0.25, ((1, 16),))
    w_keyval = bell_draw(streams_of[6], (KVLAT, HEADS * (NOPE + VDIM)), KVLAT ** -0.5, 0.375, ((1, 16),))
    w_output = bell_draw(streams_of[7], (HEADS * VDIM, D), (HEADS * VDIM) ** -0.5, 0.1875, ((1, 16),))
    moe_input = bell_draw(streams_of[8], (TOK_B, D), 1.0, 6.0, ((0, 16),))
    moe_gain = jnp.clip(1.0 + 0.18 * jax.random.normal(streams_of[9], (D,), jnp.float32), 0.1, 1.9)
    routes_keys = jax.random.split(jax.random.fold_in(streams_of[10], 1), TOK_B // MOE_DEV)
    routes_turns = jax.random.permutation(jax.random.fold_in(streams_of[10], 3), TOK_B // MOE_DEV)
    routes = jax.vmap(lambda own, number: routed_block(jax.random.fold_in(streams_of[10], 2), own, number, MOE_DEV, EXPERTS, TOP, CAP, 1))(routes_keys, routes_turns).reshape((TOK_B, TOP))
    route_weight = jnp.clip(0.25 + 1.75 * jax.random.uniform(streams_of[11], (TOK_B, TOP), jnp.float32) ** block_scale(streams_of[11], (TOK_B, TOP), ((0, 16),), -0.2, 0.2), 0.25, 2.0)
    expert_gate = bell_draw(streams_of[12], (EXPERTS, D, FE), D ** -0.5, 0.125, ((0, 16), (2, 16)))
    expert_up = bell_draw(streams_of[13], (EXPERTS, D, FE), D ** -0.5, 0.125, ((0, 16), (2, 16)))
    expert_down = bell_draw(streams_of[14], (EXPERTS, FE, D), FE ** -0.5, 0.09375, ((0, 16), (1, 16)))
    shared_gate = bell_draw(streams_of[15], (D, FS), D ** -0.5, 0.125, ((1, 16),))
    shared_up = bell_draw(streams_of[16], (D, FS), D ** -0.5, 0.125, ((1, 16),))
    shared_down = bell_draw(streams_of[17], (FS, D), FS ** -0.5, 0.125, ((0, 16),))
    return dict(q_latent=q_latent, kv_latent=kv_latent, rope_key=rope_key, q_gain=q_gain, kv_gain=kv_gain, w_query=w_query, w_keyval=w_keyval, w_output=w_output, moe_input=moe_input, moe_gain=moe_gain, routes=routes, route_weight=route_weight, expert_gate=expert_gate, expert_up=expert_up, expert_down=expert_down, shared_gate=shared_gate, shared_up=shared_up, shared_down=shared_down)


norm_eps = 1e-06
layer_eps = 1e-05
rotary_base = 10000.0
floor_value = -1e+30

def rms_scale(values, gain):
    widened = values.astype(jnp.float32)
    return (widened * lax.rsqrt(lax.optimization_barrier(jnp.mean(widened * widened, -1, keepdims=True)) + norm_eps) * gain).astype(jnp.bfloat16)

def layer_scale(values, gain):
    widened = values.astype(jnp.float32)
    centred = widened - lax.optimization_barrier(jnp.mean(widened, -1, keepdims=True))
    return (centred * lax.rsqrt(lax.optimization_barrier(jnp.mean(centred * centred, -1, keepdims=True)) + layer_eps) * gain).astype(jnp.bfloat16)

def rotary_tables(positions):
    halfway = ROPE_DIM // 2
    inverse = rotary_base ** (-(jnp.arange(halfway, dtype=jnp.float32) * 2.0 / ROPE_DIM))
    angles = positions.astype(jnp.float32)[:, None] * inverse[None, :]
    return (jnp.cos(angles), jnp.sin(angles))

def rotate(values, cosine_table, sine_table):
    halfway = values.shape[-1] // 2
    first_half = values[..., :halfway]
    second_half = values[..., halfway:]
    return jnp.concatenate([first_half * cosine_table - second_half * sine_table, second_half * cosine_table + first_half * sine_table], -1)

def merge_block(carried, stats):
    running_max, running_sum, running_acc = carried
    block_max, block_sum, attended = stats
    new_max = jnp.maximum(running_max, block_max)
    old_weight = jnp.exp(running_max - new_max)
    new_weight = jnp.exp(block_max - new_max)
    return (new_max, running_sum * old_weight + block_sum * new_weight, running_acc * old_weight[..., None] + attended.astype(jnp.float32) * new_weight[..., None])

def group_sum(hidden, down_weight, group_width):

    def add_group(group_index, total):
        hidden_cols = lax.dynamic_slice_in_dim(hidden, group_index * group_width, group_width, 1)
        weight_rows = lax.dynamic_slice_in_dim(down_weight, group_index * group_width, group_width, 0)
        product = jnp.dot(hidden_cols, weight_rows, preferred_element_type=jnp.float32)
        return total + lax.optimization_barrier(product.astype(jnp.bfloat16)).astype(jnp.float32)
    return lax.fori_loop(0, N_TP, add_group, jnp.zeros((hidden.shape[0], down_weight.shape[1]), jnp.float32))

def reference(q_latent, kv_latent, rope_key, q_gain, kv_gain, w_query, w_keyval, w_output, moe_input, moe_gain, routes, route_weight, expert_gate, expert_up, expert_down, shared_gate, shared_up, shared_down):
    positions = jnp.arange(TOK_A, dtype=jnp.int32)
    cosine_table, sine_table = rotary_tables(positions)
    q_normed = rms_scale(q_latent, q_gain)
    kv_normed = rms_scale(kv_latent, kv_gain)
    key_rot = rotate(rope_key.astype(jnp.float32), cosine_table, sine_table).astype(jnp.bfloat16)
    projected = jnp.dot(q_normed, w_query, preferred_element_type=jnp.float32).reshape(TOK_A, HEADS, NOPE + ROPE_DIM)
    queries = jnp.concatenate([projected[..., :NOPE], rotate(projected[..., NOPE:], cosine_table[:, None, :], sine_table[:, None, :])], -1).astype(jnp.bfloat16)
    keyvals = jnp.dot(kv_normed, w_keyval, preferred_element_type=jnp.float32).astype(jnp.bfloat16)
    keyvals = keyvals.reshape(TOK_A, HEADS, NOPE + VDIM)
    scale = float(NOPE + ROPE_DIM) ** (-0.5)

    def visit_group(group_index):
        first_row = group_index * TOKA_EP
        query_block = lax.dynamic_slice_in_dim(queries, first_row, TOKA_EP, 0).astype(jnp.float32)
        query_pos = first_row + jnp.arange(TOKA_EP, dtype=jnp.int32)

        def visit_block(block_index, carried):
            key_first = block_index * TOKA_EP
            keyval_block = lax.dynamic_slice_in_dim(keyvals, key_first, TOKA_EP, 0).astype(jnp.float32)
            rotated_block = lax.dynamic_slice_in_dim(key_rot, key_first, TOKA_EP, 0).astype(jnp.float32)
            key_pos = key_first + jnp.arange(TOKA_EP, dtype=jnp.int32)
            scores = jnp.einsum('qhd,khd->hqk', query_block[..., :NOPE], keyval_block[..., :NOPE])
            scores = (scores + jnp.einsum('qhd,kd->hqk', query_block[..., NOPE:], rotated_block)) * scale
            allowed = key_pos[None, :] <= query_pos[:, None]
            scores = jnp.where(allowed[None], scores, -jnp.inf)
            block_max = lax.optimization_barrier(jnp.max(scores, -1))
            weights = jnp.exp(scores - block_max[..., None])
            block_sum = lax.optimization_barrier(jnp.sum(weights, -1))
            rounded = lax.optimization_barrier(weights.astype(jnp.bfloat16)).astype(jnp.float32)
            attended = jnp.einsum('hqk,khd->qhd', rounded, keyval_block[..., NOPE:])
            attended = lax.optimization_barrier(attended.astype(jnp.bfloat16)).astype(jnp.float32)
            return merge_block(carried, (block_max.T, block_sum.T, attended))
        initial = (jnp.full((TOKA_EP, HEADS), floor_value, jnp.float32), jnp.zeros((TOKA_EP, HEADS), jnp.float32), jnp.zeros((TOKA_EP, HEADS, VDIM), jnp.float32))
        running_max, running_sum, running_acc = lax.fori_loop(0, group_index + 1, visit_block, initial)
        return (running_acc / running_sum[..., None]).astype(jnp.bfloat16).reshape(TOKA_EP, HEADS * VDIM)
    heads_out = lax.map(visit_group, jnp.arange(N_EP, dtype=jnp.int32)).reshape(TOK_A, HEADS * VDIM)
    mixed = jnp.dot(heads_out, w_output, preferred_element_type=jnp.float32).astype(jnp.bfloat16)
    block_total = TOK_B // MOE_DEV
    normed = layer_scale(moe_input, moe_gain)
    entries = routes.reshape(block_total, MOE_DEV * TOP)
    onehot = (entries[..., None] == jnp.arange(EXPERTS, dtype=jnp.int32)).astype(jnp.int32)
    earlier = jnp.cumsum(onehot, 1) - onehot
    rank_in = lax.optimization_barrier(jnp.sum(earlier * onehot, -1))
    block_ids = jnp.broadcast_to(jnp.arange(block_total, dtype=jnp.int32)[:, None], entries.shape)
    token_ids = (jnp.arange(TOK_B * TOP, dtype=jnp.int32) // TOP).reshape(block_total, MOE_DEV * TOP)
    table = jnp.full((EXPERTS, block_total, CAP), -1, jnp.int32).at[entries, block_ids, rank_in].set(token_ids)

    def run_expert(operands):
        slot_token, gate_weight, up_weight, down_weight = operands
        inputs = jnp.where((slot_token >= 0)[:, None], normed[jnp.maximum(slot_token, 0)], jnp.zeros((), jnp.bfloat16))
        hidden = jax.nn.silu(jnp.dot(inputs, gate_weight, preferred_element_type=jnp.float32))
        hidden = (hidden * jnp.dot(inputs, up_weight, preferred_element_type=jnp.float32)).astype(jnp.bfloat16)
        return group_sum(hidden, down_weight, FE_PART)
    expert_sums = lax.map(run_expert, (table.reshape(EXPERTS, block_total * CAP), expert_gate, expert_up, expert_down))
    slot_of = ((entries * block_total + block_ids) * CAP + rank_in).reshape(TOK_B, TOP)
    picked = expert_sums.reshape(EXPERTS * block_total * CAP, D)[slot_of]
    routed = lax.optimization_barrier(jnp.sum(route_weight[..., None] * picked, 1))
    shared_hidden = jax.nn.silu(jnp.dot(normed, shared_gate, preferred_element_type=jnp.float32))
    shared_hidden = (shared_hidden * jnp.dot(normed, shared_up, preferred_element_type=jnp.float32)).astype(jnp.bfloat16)
    shared_total = group_sum(shared_hidden, shared_down, FS_PART)
    moe_out = (routed + shared_total).astype(jnp.bfloat16)
    return (mixed, moe_out)
```

```python
import functools

import jax
import jax.numpy as jnp
from jax import lax
from jax.experimental import pallas as pl
from jax.experimental.pallas import tpu as pltpu
from jax.sharding import PartitionSpec as P


NOPE = 64
ROPE_DIM = 32
VDIM = 64
QK = NOPE + ROPE_DIM
MOE_DEV = 32
CAP = 6
LOG2E = 1.4426950408889634
NORM_EPS = 1e-06
LAYER_EPS = 1e-05
FLOOR = -1e30
F32 = jnp.float32
BF16 = jnp.bfloat16
SCALE = float(QK) ** (-0.5) * LOG2E
QT = 256
BLOCK = QK + VDIM


def dot0(a, b):
    return lax.dot_general(a, b, (((0,), (0,)), ((), ())), preferred_element_type=F32)


def dot(a, b):
    return jnp.dot(a, b, preferred_element_type=F32)


def vmem(n):
    return [pl.BlockSpec(memory_space=pltpu.VMEM) for _ in range(n)]


def limit(mib=24):
    return pltpu.CompilerParams(vmem_limit_bytes=mib * 1024 * 1024)


def smem():
    return pl.BlockSpec(memory_space=pltpu.SMEM)


def rms_scale(values, gain):
    widened = values.astype(F32)
    return (widened * lax.rsqrt(jnp.mean(widened * widened, -1, keepdims=True) + NORM_EPS) * gain).astype(BF16)


def dot11(a, b):
    return lax.dot_general(a, b, (((1,), (1,)), ((), ())), preferred_element_type=F32)


def rotate_rows(values, cosine, sine):
    half = ROPE_DIM // 2
    first, second = values[:half], values[half:]
    return jnp.concatenate([first * cosine - second * sine, second * cosine + first * sine], 0)


def prepare_kernel(q_ref, qg_ref, wq_ref, kvg_ref, wkv_ref, cos_ref, sin_ref, kv_ref, rope_ref, both_ref, out_ref):
    cosine, sine = cos_ref[...], sin_ref[...]
    projected = dot11(wq_ref[...], rms_scale(q_ref[...], qg_ref[...]))
    both_ref[:NOPE, :] = projected[:NOPE].astype(BF16)
    both_ref[NOPE:QK, :] = rotate_rows(projected[NOPE:], cosine, sine).astype(BF16)
    keyvals = dot11(wkv_ref[...], rms_scale(kv_ref[...], kvg_ref[...])).astype(BF16)
    rotated = rotate_rows(rope_ref[...].astype(F32), cosine, sine).astype(BF16)
    for ref, base in ((both_ref, QK), (out_ref, 0)):
        ref[base : base + NOPE, :] = keyvals[:NOPE]
        ref[base + NOPE : base + QK, :] = rotated
        ref[base + QK : base + BLOCK, :] = keyvals[NOPE:]


def prepare(q_latent, q_gain, wq, kv_gain, wkv, cosine, sine, kv, rope):
    rows = q_latent.shape[0]
    return pl.pallas_call(
        prepare_kernel,
        in_specs=vmem(9),
        out_specs=vmem(2),
        out_shape=(jax.ShapeDtypeStruct((QK + BLOCK, rows), BF16), jax.ShapeDtypeStruct((BLOCK, rows), BF16)),
        compiler_params=limit(58),
        cost_estimate=pl.CostEstimate(flops=1_500_000_000, bytes_accessed=3_000_000, transcendentals=0),
    )(q_latent, q_gain.reshape(1, -1), wq, kv_gain.reshape(1, -1), wkv, cosine, sine, kv, rope)


def attend_parts(parts, q_ref, m_ref, acc_ref):
    steps = [(part, j) for part in parts for j in range(q_ref.shape[1] // QT)]

    def score(step):
        (read, widths, _, _), j = step
        return dot0(read(0, QK, widths[j]), q_ref[:QK, j * QT : (j + 1) * QT])

    values = {}
    ahead = score(steps[0])
    for n, (part, j) in enumerate(steps):
        raw = ahead
        if n + 1 < len(steps):
            ahead = score(steps[n + 1])
        read, widths, diagonal, first = part
        cols = slice(j * QT, (j + 1) * QT)
        scores = raw * SCALE
        if diagonal:
            key_at = lax.broadcasted_iota(jnp.int32, scores.shape, 0)
            query_at = lax.broadcasted_iota(jnp.int32, scores.shape, 1) + j * QT
            scores = jnp.where(key_at <= query_at, scores, -jnp.inf)
        m_new = jnp.max(scores, 0, keepdims=True)
        if not first:
            m_old = m_ref[:, cols]
            m_new = jnp.maximum(m_new, m_old)
        weights = jnp.exp2(scores - m_new).astype(BF16)
        key = (id(part), widths[j])
        if key not in values:
            values[key] = jnp.concatenate([read(QK, BLOCK, widths[j]), jnp.ones((16, widths[j]), BF16)], 0)
        sums = dot(values[key], weights)
        if not first:
            sums = acc_ref[:, cols] * jnp.exp2(m_old - m_new) + sums
        acc_ref[:, cols] = sums
        m_ref[:, cols] = m_new


def reader(ref, base):
    return lambda start, stop, width: ref[base + start : base + stop, :width]


def full(ref, base=0):
    tiles = ref.shape[1] // QT
    return (reader(ref, base), (ref.shape[1],) * tiles, False, False)


def own_kernel(at_ref, both_ref, other_ref, m_ref, acc_ref):
    tiles = both_ref.shape[1] // QT
    widths = tuple((j + 1) * QT for j in range(tiles))
    attend_parts([(reader(both_ref, QK), widths, True, True)], both_ref, m_ref, acc_ref)

    @pl.when(at_ref[2] == 1)
    def _():
        attend_parts([full(other_ref)], both_ref, m_ref, acc_ref)


def stage_parts(stage_ref):
    return [full(stage_ref), full(stage_ref, BLOCK)]


def pairs_kernel(first, at_ref, both_ref, *refs):
    kvs, (m_in, acc_in, m_ref, acc_ref, stage_ref) = refs[:-5], refs[-5:]
    m_ref[...] = m_in[...]
    acc_ref[...] = acc_in[...]
    count = len(kvs) // 2

    def add(k, carry):
        for n in range(count):

            @pl.when(k == n)
            def _():
                stage_ref[:BLOCK, :] = kvs[2 * n][...]
                stage_ref[BLOCK:, :] = kvs[2 * n + 1][...]

        attend_parts(stage_parts(stage_ref), both_ref, m_ref, acc_ref)
        return carry

    lax.fori_loop(0, jnp.clip(at_ref[0] // 2 - first + 1, 0, count), add, 0)


def help_kernel(at_ref, q_ref, both_ref, *refs):
    kvs, (out_ref, m_ref, acc_ref, stage_ref) = refs[:-4], refs[-4:]
    at = at_ref[0] // 2
    own_other, near1, near1x, near2, near2x, extra1, extra1x, extra2, extra2x = kvs

    @pl.when(at <= 2)
    def _():
        m_ref[...] = jnp.full(m_ref.shape, FLOOR, F32)
        acc_ref[...] = jnp.zeros(acc_ref.shape, F32)

        def add(n, carry):
            picks = (
                ((n == 0) & (at <= 1), both_ref, own_other, QK),
                ((n == 0) & (at == 2), near2, near2x, 0),
                ((n == 1) & (at == 1), near1, near1x, 0),
                ((n == 1) & (at == 0), extra1, extra1x, 0),
                ((n == 2) & (at == 0), extra2, extra2x, 0),
            )
            for live, ref, pair_ref, base in picks:

                @pl.when(live)
                def _():
                    stage_ref[:BLOCK, :] = ref[base : base + BLOCK, :]
                    stage_ref[BLOCK:, :] = pair_ref[...]

            attend_parts(stage_parts(stage_ref), q_ref, m_ref, acc_ref)
            return carry

        lax.fori_loop(0, 3 - at, add, 0)
        out_ref[:VDIM, :] = acc_ref[:VDIM, :]
        tail = acc_ref[VDIM : VDIM + 8, :]
        row = lax.broadcasted_iota(jnp.int32, tail.shape, 0)
        out_ref[VDIM:, :] = jnp.where(row == 1, m_ref[...], tail)


def merge_kernel(at_ref, help_ref, m_ref, acc_ref, out_ref):
    helped = at_ref[0] // 2 >= 5
    m_old = m_ref[...]
    m_other = jnp.where(helped, help_ref[VDIM + 1 : VDIM + 2, :], FLOOR)
    m_new = jnp.maximum(m_old, m_other)
    other = jnp.where(helped, help_ref[: VDIM + 1, :], 0.0)
    acc = acc_ref[: VDIM + 1, :] * jnp.exp2(m_old - m_new) + other * jnp.exp2(m_other - m_new)
    out_ref[...] = (acc[:VDIM] / acc[VDIM:]).astype(BF16)


def state_shapes(rows):
    return (jax.ShapeDtypeStruct((1, rows), F32), jax.ShapeDtypeStruct((VDIM + 16, rows), F32))


def state_scratch(rows):
    return [pltpu.VMEM((1, rows), F32), pltpu.VMEM((VDIM + 16, rows), F32)] + stage(rows)


def stage(rows):
    return [pltpu.VMEM((2 * BLOCK, rows), BF16)]


def attend(kernel, flops, at, args, out_shape, scratch=()):
    many = isinstance(out_shape, tuple)
    return pl.pallas_call(
        kernel,
        in_specs=[smem()] + vmem(len(args)),
        out_specs=vmem(len(out_shape)) if many else pl.BlockSpec(memory_space=pltpu.VMEM),
        out_shape=out_shape,
        scratch_shapes=list(scratch),
        compiler_params=limit(),
        cost_estimate=pl.CostEstimate(flops=flops, bytes_accessed=1_000_000, transcendentals=0),
    )(at, *args)


def heads_kernel(at_ref, w_ref, w2_ref, *refs):
    pieces, (own_ref, other_ref) = refs[:-2], refs[-2:]
    count = len(pieces)
    z, core = at_ref[1], at_ref[2]
    starts = [pl.multiple_of((((z + count - k) % count) * 2 + core) * VDIM, VDIM) for k in range(count)]
    stacked = jnp.concatenate([piece[...] for piece in pieces], 0)
    pick = lambda ref: jnp.concatenate([ref[pl.ds(s, VDIM), :] for s in starts], 0)
    other_ref[...] = dot0(stacked, pick(w2_ref)).astype(BF16)
    own_ref[...] = dot0(stacked, pick(w_ref))


def project_heads(at, w, w2, pieces):
    shape = (pieces[0].shape[1], w.shape[1])
    return pl.pallas_call(
        heads_kernel,
        in_specs=[smem()] + vmem(2 + len(pieces)),
        out_specs=vmem(2),
        out_shape=(jax.ShapeDtypeStruct(shape, F32), jax.ShapeDtypeStruct(shape, BF16)),
        compiler_params=limit(),
        cost_estimate=pl.CostEstimate(flops=500_000_000, bytes_accessed=3_000_000, transcendentals=0),
    )(at, w, w2, *pieces)


def layer_scale(values, gain):
    widened = values.astype(F32)
    centred = widened - jnp.mean(widened, -1, keepdims=True)
    return (centred * lax.rsqrt(jnp.mean(centred * centred, -1, keepdims=True) + LAYER_EPS) * gain).astype(BF16)


def slot_matrix(at_ref, routes_ref, weight_ref, experts):
    count = at_ref.shape[0]
    tokens = count * MOE_DEV
    every = routes_ref.shape[1]
    col = lax.broadcasted_iota(jnp.int32, (1, tokens), 1)
    block = jnp.zeros((1, tokens), jnp.int32)
    for b in range(count):
        block = jnp.where(col // MOE_DEV == b, at_ref[b], block)
    token = block * MOE_DEV + col % MOE_DEV
    pick = (lax.broadcasted_iota(jnp.int32, (every, tokens), 0) == token).astype(BF16)
    named = dot(routes_ref[...].astype(BF16), pick)
    ids = lax.broadcasted_iota(jnp.int32, (experts, tokens), 0).astype(F32)
    first, second = (ids == named[0:1]).astype(F32), (ids == named[1:2]).astype(F32)
    chosen = (first + second).astype(BF16)
    value = chosen
    if weight_ref is not None:
        weight = dot(weight_ref[...].astype(BF16), pick)
        value = (first * weight[0:1] + second * weight[1:2]).astype(BF16)
    src = lax.broadcasted_iota(jnp.int32, (tokens, tokens), 0)
    dst = lax.broadcasted_iota(jnp.int32, (tokens, tokens), 1)
    earlier = ((src < dst) & (src // MOE_DEV == dst // MOE_DEV)).astype(BF16)
    place = dot(chosen, earlier) + (block // 4 * CAP).astype(F32)
    per = count * CAP
    shape = (experts * per, experts)
    expand = (lax.broadcasted_iota(jnp.int32, shape, 0) // per == lax.broadcasted_iota(jnp.int32, shape, 1)).astype(BF16)
    spread = dot(expand, value)
    slot = (lax.broadcasted_iota(jnp.int32, spread.shape, 0) % per).astype(F32)
    return jnp.where(dot(expand, place.astype(BF16)) == slot, spread, 0.0).astype(BF16)


def dispatch_kernel(experts, count, blocks_ref, gain_ref, routes_ref, *refs):
    x_refs, out_ref = refs[:count], refs[count]
    normed = layer_scale(jnp.concatenate([r[...] for r in x_refs], 0), gain_ref[...])
    out_ref[...] = dot(slot_matrix(blocks_ref, routes_ref, None, experts), normed).astype(BF16)


def dispatch(moe_input, gain, routes_t, blocks, experts):
    width = moe_input.shape[1]
    count = blocks.shape[0]
    rows = experts * count * CAP
    block_spec = lambda b: pl.BlockSpec((MOE_DEV, width), lambda i, s: (s[b], 0))
    return pl.pallas_call(
        functools.partial(dispatch_kernel, experts, count),
        grid_spec=pltpu.PrefetchScalarGridSpec(
            num_scalar_prefetch=1,
            grid=(1,),
            in_specs=[
                pl.BlockSpec((1, width), lambda i, s: (0, 0)),
                pl.BlockSpec(routes_t.shape, lambda i, s: (0, 0)),
            ]
            + [block_spec(b) for b in range(count)],
            out_specs=pl.BlockSpec((rows, width), lambda i, s: (0, 0)),
        ),
        out_shape=jax.ShapeDtypeStruct((rows, width), BF16),
        compiler_params=limit(),
        cost_estimate=pl.CostEstimate(flops=400_000_000, bytes_accessed=2_000_000, transcendentals=0),
    )(blocks, gain.reshape(1, width), routes_t, *([moe_input] * count))


def shared_kernel(at_ref, x_ref, gain_ref, gate_ref, up_ref, own_ref, other_ref):
    normed = layer_scale(x_ref[...], gain_ref[...])
    hidden = (jax.nn.silu(dot(normed, gate_ref[...])) * dot(normed, up_ref[...])).astype(BF16)
    core = at_ref[2]
    blocks = hidden.shape[0] // MOE_DEV
    part = lambda parity: jnp.concatenate(
        [hidden[(2 * b + parity) * MOE_DEV : (2 * b + parity + 1) * MOE_DEV] for b in range(blocks // 2)], 0
    )
    even, odd = part(0), part(1)
    own_ref[...] = jnp.where(core == 0, even, odd)
    other_ref[...] = jnp.where(core == 0, odd, even)


def shared_hidden(at, moe_input, gain, gate, up):
    rows, width = moe_input.shape
    out = jax.ShapeDtypeStruct((rows // 2, gate.shape[1]), BF16)
    return pl.pallas_call(
        shared_kernel,
        in_specs=[smem()] + vmem(4),
        out_specs=vmem(2),
        out_shape=(out, out),
        compiler_params=limit(),
        cost_estimate=pl.CostEstimate(flops=1_500_000_000, bytes_accessed=4_000_000, transcendentals=0),
    )(at, moe_input, gain.reshape(1, width), gate, up)


def expert_kernel(count, *refs):
    xs, (gate, up, gate2, up2, down, down2), outs = refs[:count], refs[count : count + 6], refs[count + 6 :]
    x = jnp.concatenate([r[...] for r in xs], 0) if count > 1 else xs[0][...]
    hidden = lambda g, u: (jax.nn.silu(dot(x, g[...])) * dot(x, u[...])).astype(BF16)
    total = (dot(hidden(gate, up), down[...]) + dot(hidden(gate2, up2), down2[...])).astype(BF16)
    rows = outs[0].shape[0]
    for n, out_ref in enumerate(outs):
        out_ref[...] = total[n * rows : (n + 1) * rows]


def run_expert(xs, weights):
    return pl.pallas_call(
        functools.partial(expert_kernel, len(xs)),
        in_specs=vmem(len(xs) + 6),
        out_specs=vmem(len(xs)),
        out_shape=tuple(jax.ShapeDtypeStruct(x.shape, BF16) for x in xs),
        compiler_params=limit(),
        cost_estimate=pl.CostEstimate(flops=5_000_000_000, bytes_accessed=9_000_000, transcendentals=0),
    )(*xs, *weights)


def block_rows(at_ref, ref, per=2):
    starts = [pl.multiple_of(at_ref[b] // per * MOE_DEV, MOE_DEV) for b in range(at_ref.shape[0])]
    return jnp.concatenate([ref[pl.ds(s, MOE_DEV), :] for s in starts], 0)


def shared_far_kernel(at_ref, own_ref, other_ref, down_ref, down2_ref, low_ref, high_ref):
    total = dot(block_rows(at_ref, own_ref), down_ref[...]) + dot(block_rows(at_ref, other_ref), down2_ref[...])
    half = low_ref.shape[0]
    low_ref[...] = total[:half].astype(BF16)
    high_ref[...] = total[half:].astype(BF16)


def shared_far(blocks, own, other, down, down2):
    out = jax.ShapeDtypeStruct((blocks.shape[0] // 2 * MOE_DEV, down.shape[1]), BF16)
    return pl.pallas_call(
        shared_far_kernel,
        in_specs=[smem()] + vmem(4),
        out_specs=vmem(2),
        out_shape=(out, out),
        compiler_params=limit(),
        cost_estimate=pl.CostEstimate(flops=300_000_000, bytes_accessed=2_000_000, transcendentals=0),
    )(blocks, own, other, down, down2)


def combine_kernel(
    experts, at_ref, recv_ref, routes_ref, weight_ref, own_ref, other_ref, down_ref, down2_ref, low_ref, high_ref, *out_refs
):
    total = dot0(slot_matrix(at_ref, routes_ref, weight_ref, experts), recv_ref[...])
    total = total + dot(block_rows(at_ref, own_ref), down_ref[...]) + dot(block_rows(at_ref, other_ref), down2_ref[...])
    half = low_ref.shape[0] // MOE_DEV
    for b, out_ref in enumerate(out_refs):
        place = at_ref[b] // 4
        start = pl.multiple_of(place % half * MOE_DEV, MOE_DEV)
        near = jnp.where(place < half, low_ref[pl.ds(start, MOE_DEV), :], high_ref[pl.ds(start, MOE_DEV), :])
        out_ref[...] = (total[b * MOE_DEV : (b + 1) * MOE_DEV] + near.astype(F32)).astype(BF16)


def combine(received, routes_t, weight_t, blocks, own, other, down, down2, low, high, experts):
    width = received.shape[1]
    count = blocks.shape[0]
    return pl.pallas_call(
        functools.partial(combine_kernel, experts),
        in_specs=[smem()] + vmem(9),
        out_specs=vmem(count),
        out_shape=(jax.ShapeDtypeStruct((MOE_DEV, width), BF16),) * count,
        compiler_params=limit(),
        cost_estimate=pl.CostEstimate(flops=600_000_000, bytes_accessed=4_000_000, transcendentals=0),
    )(blocks, received, routes_t, weight_t, own, other, down, down2, low, high)


def sum_kernel(near_ref, low_ref, high_ref, out_ref):
    half = low_ref.shape[0]
    out_ref[:half] = (near_ref[:half].astype(F32) + low_ref[...].astype(F32)).astype(BF16)
    out_ref[half:] = (near_ref[half:].astype(F32) + high_ref[...].astype(F32)).astype(BF16)


def add_halves(near, low, high):
    return pl.pallas_call(
        sum_kernel,
        in_specs=vmem(3),
        out_specs=pl.BlockSpec(memory_space=pltpu.VMEM),
        out_shape=jax.ShapeDtypeStruct(near.shape, BF16),
        compiler_params=limit(),
        cost_estimate=pl.CostEstimate(flops=100_000_000, bytes_accessed=4_000_000, transcendentals=0),
    )(near, low, high)


def layer(
    q_latent,
    kv_latent,
    rope_key,
    q_gain,
    kv_gain,
    w_query,
    w_keyval,
    w_output,
    moe_input,
    moe_gain,
    routes,
    route_weight,
    expert_gate,
    expert_up,
    expert_down,
    shared_gate,
    shared_up,
    shared_down,
):
    ep = lax.axis_index("ep")
    tp = lax.axis_index("tp")
    n_ep, n_tp = lax.axis_size("ep"), lax.axis_size("tp")
    z, core = tp // 2, tp % 2
    n_z = n_tp // 2
    at = jnp.stack([ep, z, core]).astype(jnp.int32)
    swap = lambda v: lax.ppermute(v, "tp", [(i, i ^ 1) for i in range(n_tp)])
    ahead = lambda v, k: lax.ppermute(v, "tp", [(i, (i + 2 * k) % n_tp) for i in range(n_tp)])
    exchange = lambda v: lax.all_to_all(v, "ep", split_axis=0, concat_axis=0, tiled=True)
    rows = q_latent.shape[0]
    width = moe_input.shape[1]

    group = n_z // 2
    step = jnp.arange(group, dtype=jnp.int32)
    here, turned, beside = [o * 2 + core for o in ((z % 2) + 2 * step, (z + 2 * step) % n_z, 1 - z % 2 + 2 * step)]
    routes_t, weight_t = routes.T, route_weight.T

    send = dispatch(moe_input, moe_gain, routes_t, here, n_ep)
    near = exchange(send.reshape(n_ep, group * CAP, width)).reshape(n_ep * group * CAP, width)
    half_rows = near.shape[0] // 2
    far = [ahead(near[:half_rows], 1), ahead(near[half_rows:], -1)]

    gate, up, down = expert_gate[0], expert_up[0], expert_down[0]
    weights = (gate, up, swap(gate), swap(up), down, swap(down))
    shared_down2 = swap(shared_down)
    w_output2 = swap(w_output)

    positions = (ep * rows + jnp.arange(rows, dtype=jnp.int32)).astype(F32)
    half = ROPE_DIM // 2
    inverse = 10000.0 ** (-(jnp.arange(half, dtype=F32) * 2.0 / ROPE_DIM))
    angles = inverse[:, None] * positions[None, :]
    cosine, sine = jnp.cos(angles), jnp.sin(angles)
    both, kv_t = prepare(
        q_latent, q_gain, w_query.T, kv_gain, w_keyval.T, cosine, sine, kv_latent, rope_key.T
    )

    n_pair = n_ep // 2
    hand = lambda v, moves: lax.ppermute(
        v,
        ("ep", "tp"),
        [
            ((2 * s + b) * n_tp + 2 * h + r, (2 * d + r) * n_tp + 2 * h + b)
            for s, d in moves
            for b in range(2)
            for r in range(2)
            for h in range(n_z)
        ],
    )
    straight = lambda v, moves: lax.ppermute(v, "ep", [(2 * s + r, 2 * d + r) for s, d in moves for r in range(2)])
    home = [(p, p) for p in range(n_pair)]
    late = [(n_pair - 1 - p, p) for p in range(3)]
    both = hand(both, home)
    own_other = swap(both[QK:])
    q_help = straight(both[:QK], late)
    shifted = [hand(kv_t, [(p, p + k) for p in range(n_pair - k)]) for k in range(1, 5)]
    extra = [hand(kv_t, [(p, 0)]) for p in (1, 2)]
    blocks_of = lambda v: (v, swap(v))
    near_kv = blocks_of(shifted[0]) + blocks_of(shifted[1])
    far_kv = blocks_of(shifted[2]) + blocks_of(shifted[3])
    extra_kv = blocks_of(extra[0]) + blocks_of(extra[1])

    own_hidden, other_hidden = shared_hidden(at, moe_input, moe_gain, shared_gate, shared_up)
    other_hidden = swap(other_hidden)
    low, high = shared_far(beside, own_hidden, other_hidden, shared_down, shared_down2)
    low, high = ahead(low, 1), ahead(high, -1)

    state = attend(own_kernel, 4_000_000_000, at, (both, own_other), state_shapes(rows))
    state = attend(
        functools.partial(pairs_kernel, 1), 12_000_000_000, at, (both, *near_kv, *state), state_shapes(rows), stage(rows)
    )
    helped = attend(
        help_kernel, 6_000_000_000, at, (q_help, both, own_other, *near_kv, *extra_kv),
        jax.ShapeDtypeStruct((VDIM + 8, rows), F32), state_scratch(rows),
    )
    helped = straight(helped, [(p, q) for q, p in late])
    state = attend(
        functools.partial(pairs_kernel, 3), 12_000_000_000, at, (both, *far_kv, *state), state_shapes(rows), stage(rows)
    )
    heads = attend(merge_kernel, 100_000_000, at, (helped, *state), jax.ShapeDtypeStruct((VDIM, rows), BF16))

    (near_out,) = run_expert([near], weights)
    far_low, far_high = run_expert(far, weights)
    far_low, far_high = ahead(far_low, 1), ahead(far_high, -1)
    near_out = add_halves(near_out, far_low, far_high)
    returned = exchange(near_out.reshape(n_ep, group * CAP, width)).reshape(n_ep * group * CAP, width)

    sums = combine(
        returned, routes_t, weight_t, turned, own_hidden, other_hidden, shared_down, shared_down2, low, high, n_ep
    )
    parts = [sums[0]] + [ahead(sums[j], 2 * j) for j in range(1, group)]
    moe_out = functools.reduce(lambda a, b: a + b, [p.astype(F32) for p in parts]).astype(BF16)

    heads = hand(heads, home)
    first = {0: heads, **{k: ahead(heads, k) for k in (1, -1, 2, -2)}}
    pieces = [first[k] for k in (0, 1, 2)] + [ahead(first[2], 1), ahead(first[2], 2), ahead(first[-2], -1)]
    pieces += [first[-2], first[-1]]
    own_sum, for_other = project_heads(at, w_output, w_output2, pieces)
    mixed = (own_sum + swap(for_other).astype(F32)).astype(BF16)
    return (mixed, moe_out)


def solution(mesh):
    in_specs = (
        P("ep", None),
        P("ep", None),
        P("ep", None),
        P(),
        P(),
        P(None, "tp"),
        P(None, "tp"),
        P(None, "tp"),
        P("ep", None),
        P(),
        P("ep", None),
        P("ep", None),
        P("ep", None, "tp"),
        P("ep", None, "tp"),
        P("ep", "tp", None),
        P(None, "tp"),
        P(None, "tp"),
        P("tp", None),
    )
    out_specs = (P("ep", "tp"), P(("ep", "tp"), None))
    return jax.shard_map(layer, mesh=mesh, in_specs=in_specs, out_specs=out_specs, check_vma=False)
```

```python
import functools

import jax
import jax.numpy as jnp
from jax import lax
from jax.experimental import pallas as pl
from jax.experimental.pallas import tpu as pltpu
from jax.sharding import PartitionSpec as P


NOPE = 64
ROPE_DIM = 32
VDIM = 64
QK = NOPE + ROPE_DIM
MOE_DEV = 32
CAP = 6
LOG2E = 1.4426950408889634
NORM_EPS = 1e-06
LAYER_EPS = 1e-05
FLOOR = -1e30
F32 = jnp.float32
BF16 = jnp.bfloat16
SCALE = float(QK) ** (-0.5) * LOG2E
QT = 256
BLOCK = QK + VDIM


def dot0(a, b):
    return lax.dot_general(a, b, (((0,), (0,)), ((), ())), preferred_element_type=F32)


def dot(a, b):
    return jnp.dot(a, b, preferred_element_type=F32)


def vmem(n):
    return [pl.BlockSpec(memory_space=pltpu.VMEM) for _ in range(n)]


def limit(mib=24):
    return pltpu.CompilerParams(vmem_limit_bytes=mib * 1024 * 1024)


def smem():
    return pl.BlockSpec(memory_space=pltpu.SMEM)


def rms_scale(values, gain):
    widened = values.astype(F32)
    return (widened * lax.rsqrt(jnp.mean(widened * widened, -1, keepdims=True) + NORM_EPS) * gain).astype(BF16)


def dot11(a, b):
    return lax.dot_general(a, b, (((1,), (1,)), ((), ())), preferred_element_type=F32)


def rotate_rows(values, cosine, sine):
    half = ROPE_DIM // 2
    first, second = values[:half], values[half:]
    return jnp.concatenate([first * cosine - second * sine, second * cosine + first * sine], 0)


def prepare_kernel(q_ref, qg_ref, wq_ref, kvg_ref, wkv_ref, cos_ref, sin_ref, kv_ref, rope_ref, both_ref, out_ref):
    cosine, sine = cos_ref[...], sin_ref[...]
    projected = dot11(wq_ref[...], rms_scale(q_ref[...], qg_ref[...]))
    both_ref[:NOPE, :] = projected[:NOPE].astype(BF16)
    both_ref[NOPE:QK, :] = rotate_rows(projected[NOPE:], cosine, sine).astype(BF16)
    keyvals = dot11(wkv_ref[...], rms_scale(kv_ref[...], kvg_ref[...])).astype(BF16)
    rotated = rotate_rows(rope_ref[...].astype(F32), cosine, sine).astype(BF16)
    for ref, base in ((both_ref, QK), (out_ref, 0)):
        ref[base : base + NOPE, :] = keyvals[:NOPE]
        ref[base + NOPE : base + QK, :] = rotated
        ref[base + QK : base + BLOCK, :] = keyvals[NOPE:]


def prepare(q_latent, q_gain, wq, kv_gain, wkv, cosine, sine, kv, rope):
    rows = q_latent.shape[0]
    return pl.pallas_call(
        prepare_kernel,
        in_specs=vmem(9),
        out_specs=vmem(2),
        out_shape=(jax.ShapeDtypeStruct((QK + BLOCK, rows), BF16), jax.ShapeDtypeStruct((BLOCK, rows), BF16)),
        compiler_params=limit(58),
        cost_estimate=pl.CostEstimate(flops=1_500_000_000, bytes_accessed=3_000_000, transcendentals=0),
    )(q_latent, q_gain.reshape(1, -1), wq, kv_gain.reshape(1, -1), wkv, cosine, sine, kv, rope)


def attend_parts(parts, q_ref, m_ref, acc_ref):
    steps = [(part, j) for part in parts for j in range(q_ref.shape[1] // QT)]

    def score(step):
        (read, widths, _, _), j = step
        return dot0(read(0, QK, widths[j]), q_ref[:QK, j * QT : (j + 1) * QT])

    values = {}
    ahead = score(steps[0])
    for n, (part, j) in enumerate(steps):
        raw = ahead
        if n + 1 < len(steps):
            ahead = score(steps[n + 1])
        read, widths, diagonal, first = part
        cols = slice(j * QT, (j + 1) * QT)
        scores = raw * SCALE
        if diagonal:
            key_at = lax.broadcasted_iota(jnp.int32, scores.shape, 0)
            query_at = lax.broadcasted_iota(jnp.int32, scores.shape, 1) + j * QT
            scores = jnp.where(key_at <= query_at, scores, -jnp.inf)
        m_new = jnp.max(scores, 0, keepdims=True)
        if not first:
            m_old = m_ref[:, cols]
            m_new = jnp.maximum(m_new, m_old)
        weights = jnp.exp2(scores - m_new).astype(BF16)
        key = (id(part), widths[j])
        if key not in values:
            values[key] = jnp.concatenate([read(QK, BLOCK, widths[j]), jnp.ones((16, widths[j]), BF16)], 0)
        sums = dot(values[key], weights)
        if not first:
            sums = acc_ref[:, cols] * jnp.exp2(m_old - m_new) + sums
        acc_ref[:, cols] = sums
        m_ref[:, cols] = m_new


def reader(ref, base):
    return lambda start, stop, width: ref[base + start : base + stop, :width]


def full(ref, base=0):
    tiles = ref.shape[1] // QT
    return (reader(ref, base), (ref.shape[1],) * tiles, False, False)


def own_kernel(at_ref, both_ref, other_ref, m_ref, acc_ref):
    tiles = both_ref.shape[1] // QT
    widths = tuple((j + 1) * QT for j in range(tiles))
    attend_parts([(reader(both_ref, QK), widths, True, True)], both_ref, m_ref, acc_ref)

    @pl.when(at_ref[2] == 1)
    def _():
        attend_parts([full(other_ref)], both_ref, m_ref, acc_ref)


def stage_parts(stage_ref):
    return [full(stage_ref), full(stage_ref, BLOCK)]


def pairs_kernel(first, at_ref, both_ref, *refs):
    kvs, (m_in, acc_in, m_ref, acc_ref, stage_ref) = refs[:-5], refs[-5:]
    m_ref[...] = m_in[...]
    acc_ref[...] = acc_in[...]
    count = len(kvs) // 2

    def add(k, carry):
        for n in range(count):

            @pl.when(k == n)
            def _():
                stage_ref[:BLOCK, :] = kvs[2 * n][...]
                stage_ref[BLOCK:, :] = kvs[2 * n + 1][...]

        attend_parts(stage_parts(stage_ref), both_ref, m_ref, acc_ref)
        return carry

    lax.fori_loop(0, jnp.clip(at_ref[0] // 2 - first + 1, 0, count), add, 0)


def help_kernel(at_ref, q_ref, both_ref, *refs):
    kvs, (out_ref, m_ref, acc_ref, stage_ref, help_ref, sem) = refs[:-6], refs[-6:]
    at = at_ref[0] // 2

    def fetch(source, target):
        copy = pltpu.make_async_copy(source, target, sem)
        copy.start()
        copy.wait()

    own_other, near1, near1x, near2, near2x, extra1, extra1x, extra2, extra2x = kvs

    @pl.when(at <= 2)
    def _():
        fetch(q_ref, help_ref)
        m_ref[...] = jnp.full(m_ref.shape, FLOOR, F32)
        acc_ref[...] = jnp.zeros(acc_ref.shape, F32)

        def add(n, carry):
            picks = (
                ((n == 0) & (at <= 1), both_ref, own_other, QK),
                ((n == 0) & (at == 2), near2, near2x, 0),
                ((n == 1) & (at == 1), near1, near1x, 0),
            )
            for live, ref, pair_ref in (
                ((n == 1) & (at == 0), extra1, extra1x),
                ((n == 2) & (at == 0), extra2, extra2x),
            ):

                @pl.when(live)
                def _():
                    fetch(ref, stage_ref.at[:BLOCK, :])
                    fetch(pair_ref, stage_ref.at[BLOCK:, :])

            for live, ref, pair_ref, base in picks:

                @pl.when(live)
                def _():
                    stage_ref[:BLOCK, :] = ref[base : base + BLOCK, :]
                    stage_ref[BLOCK:, :] = pair_ref[...]

            attend_parts(stage_parts(stage_ref), help_ref, m_ref, acc_ref)
            return carry

        lax.fori_loop(0, 3 - at, add, 0)
        out_ref[:VDIM, :] = acc_ref[:VDIM, :]
        tail = acc_ref[VDIM : VDIM + 8, :]
        row = lax.broadcasted_iota(jnp.int32, tail.shape, 0)
        out_ref[VDIM:, :] = jnp.where(row == 1, m_ref[...], tail)


def merge_kernel(at_ref, help_ref, m_ref, acc_ref, out_ref):
    helped = at_ref[0] // 2 >= 5
    m_old = m_ref[...]
    m_other = jnp.where(helped, help_ref[VDIM + 1 : VDIM + 2, :], FLOOR)
    m_new = jnp.maximum(m_old, m_other)
    other = jnp.where(helped, help_ref[: VDIM + 1, :], 0.0)
    acc = acc_ref[: VDIM + 1, :] * jnp.exp2(m_old - m_new) + other * jnp.exp2(m_other - m_new)
    out_ref[...] = (acc[:VDIM] / acc[VDIM:]).astype(BF16)


def state_shapes(rows):
    return (jax.ShapeDtypeStruct((1, rows), F32), jax.ShapeDtypeStruct((VDIM + 16, rows), F32))


def state_scratch(rows):
    return [pltpu.VMEM((1, rows), F32), pltpu.VMEM((VDIM + 16, rows), F32)] + stage(rows)


def stage(rows):
    return [pltpu.VMEM((2 * BLOCK, rows), BF16)]


def attend(kernel, flops, at, args, out_shape, scratch=(), away=()):
    many = isinstance(out_shape, tuple)
    return pl.pallas_call(
        kernel,
        in_specs=[smem()]
        + [pl.BlockSpec(memory_space=pl.ANY if n in away else pltpu.VMEM) for n in range(len(args))],
        out_specs=vmem(len(out_shape)) if many else pl.BlockSpec(memory_space=pltpu.VMEM),
        out_shape=out_shape,
        scratch_shapes=list(scratch),
        compiler_params=limit(),
        cost_estimate=pl.CostEstimate(flops=flops, bytes_accessed=1_000_000, transcendentals=0),
    )(at, *args)


def heads_kernel(at_ref, w_ref, w2_ref, *refs):
    pieces, (own_ref, other_ref) = refs[:-2], refs[-2:]
    count = len(pieces)
    z, core, parity = at_ref[1], at_ref[2], at_ref[0] % 2
    starts = [pl.multiple_of((((z + count - k) % count) * 2 + parity) * VDIM, VDIM) for k in range(count)]
    stacked = jnp.concatenate([piece[...] for piece in pieces], 0)
    pick = lambda ref: jnp.concatenate([ref[pl.ds(s, VDIM), :] for s in starts], 0)
    here, there = pick(w_ref), pick(w2_ref)
    own_ref[...] = dot0(stacked, jnp.where(core == parity, here, there)).astype(BF16)
    other_ref[...] = dot0(stacked, jnp.where(core == parity, there, here)).astype(BF16)


def project_heads(at, w, w2, pieces):
    shape = (pieces[0].shape[1], w.shape[1])
    return pl.pallas_call(
        heads_kernel,
        in_specs=[smem()] + vmem(2 + len(pieces)),
        out_specs=vmem(2),
        out_shape=(jax.ShapeDtypeStruct(shape, BF16),) * 2,
        compiler_params=limit(),
        cost_estimate=pl.CostEstimate(flops=500_000_000, bytes_accessed=3_000_000, transcendentals=0),
    )(at, w, w2, *pieces)


def layer_scale(values, gain):
    widened = values.astype(F32)
    centred = widened - jnp.mean(widened, -1, keepdims=True)
    return (centred * lax.rsqrt(jnp.mean(centred * centred, -1, keepdims=True) + LAYER_EPS) * gain).astype(BF16)


def slot_matrix(at_ref, routes_ref, weight_ref, experts):
    count = at_ref.shape[0]
    tokens = count * MOE_DEV
    every = routes_ref.shape[1]
    col = lax.broadcasted_iota(jnp.int32, (1, tokens), 1)
    block = jnp.zeros((1, tokens), jnp.int32)
    for b in range(count):
        block = jnp.where(col // MOE_DEV == b, at_ref[b], block)
    token = block * MOE_DEV + col % MOE_DEV
    pick = (lax.broadcasted_iota(jnp.int32, (every, tokens), 0) == token).astype(BF16)
    named = dot(routes_ref[...].astype(BF16), pick)
    ids = lax.broadcasted_iota(jnp.int32, (experts, tokens), 0).astype(F32)
    first, second = (ids == named[0:1]).astype(F32), (ids == named[1:2]).astype(F32)
    chosen = (first + second).astype(BF16)
    value = chosen
    if weight_ref is not None:
        weight = dot(weight_ref[...].astype(BF16), pick)
        value = (first * weight[0:1] + second * weight[1:2]).astype(BF16)
    src = lax.broadcasted_iota(jnp.int32, (tokens, tokens), 0)
    dst = lax.broadcasted_iota(jnp.int32, (tokens, tokens), 1)
    earlier = ((src < dst) & (src // MOE_DEV == dst // MOE_DEV)).astype(BF16)
    place = dot(chosen, earlier) + (block // 4 * CAP).astype(F32)
    per = count * CAP
    shape = (experts * per, experts)
    expand = (lax.broadcasted_iota(jnp.int32, shape, 0) // per == lax.broadcasted_iota(jnp.int32, shape, 1)).astype(BF16)
    spread = dot(expand, value)
    slot = (lax.broadcasted_iota(jnp.int32, spread.shape, 0) % per).astype(F32)
    return jnp.where(dot(expand, place.astype(BF16)) == slot, spread, 0.0).astype(BF16)


def dispatch_kernel(experts, count, blocks_ref, gain_ref, routes_ref, *refs):
    x_refs, out_ref = refs[:count], refs[count]
    normed = layer_scale(jnp.concatenate([r[...] for r in x_refs], 0), gain_ref[...])
    out_ref[...] = dot(slot_matrix(blocks_ref, routes_ref, None, experts), normed).astype(BF16)


def dispatch(moe_input, gain, routes_t, blocks, experts):
    width = moe_input.shape[1]
    count = blocks.shape[0]
    rows = experts * count * CAP
    block_spec = lambda b: pl.BlockSpec((MOE_DEV, width), lambda i, s: (s[b], 0))
    return pl.pallas_call(
        functools.partial(dispatch_kernel, experts, count),
        grid_spec=pltpu.PrefetchScalarGridSpec(
            num_scalar_prefetch=1,
            grid=(1,),
            in_specs=[
                pl.BlockSpec((1, width), lambda i, s: (0, 0)),
                pl.BlockSpec(routes_t.shape, lambda i, s: (0, 0)),
            ]
            + [block_spec(b) for b in range(count)],
            out_specs=pl.BlockSpec((rows, width), lambda i, s: (0, 0)),
        ),
        out_shape=jax.ShapeDtypeStruct((rows, width), BF16),
        compiler_params=limit(),
        cost_estimate=pl.CostEstimate(flops=400_000_000, bytes_accessed=2_000_000, transcendentals=0),
    )(blocks, gain.reshape(1, width), routes_t, *([moe_input] * count))


def shared_kernel(at_ref, x_ref, gain_ref, gate_ref, up_ref, own_ref, other_ref):
    normed = layer_scale(x_ref[...], gain_ref[...])
    hidden = (jax.nn.silu(dot(normed, gate_ref[...])) * dot(normed, up_ref[...])).astype(BF16)
    core = at_ref[2]
    blocks = hidden.shape[0] // MOE_DEV
    part = lambda parity: jnp.concatenate(
        [hidden[(2 * b + parity) * MOE_DEV : (2 * b + parity + 1) * MOE_DEV] for b in range(blocks // 2)], 0
    )
    even, odd = part(0), part(1)
    own_ref[...] = jnp.where(core == 0, even, odd)
    other_ref[...] = jnp.where(core == 0, odd, even)


def shared_hidden(at, moe_input, gain, gate, up):
    rows, width = moe_input.shape
    out = jax.ShapeDtypeStruct((rows // 2, gate.shape[1]), BF16)
    return pl.pallas_call(
        shared_kernel,
        in_specs=[smem()] + vmem(4),
        out_specs=vmem(2),
        out_shape=(out, out),
        compiler_params=limit(),
        cost_estimate=pl.CostEstimate(flops=1_500_000_000, bytes_accessed=4_000_000, transcendentals=0),
    )(at, moe_input, gain.reshape(1, width), gate, up)


def expert_kernel(count, *refs):
    xs, (gate, up, gate2, up2, down, down2), outs = refs[:count], refs[count : count + 6], refs[count + 6 :]
    x = jnp.concatenate([r[...] for r in xs], 0) if count > 1 else xs[0][...]
    hidden = lambda g, u: (jax.nn.silu(dot(x, g[...])) * dot(x, u[...])).astype(BF16)
    total = (dot(hidden(gate, up), down[...]) + dot(hidden(gate2, up2), down2[...])).astype(BF16)
    rows = outs[0].shape[0]
    for n, out_ref in enumerate(outs):
        out_ref[...] = total[n * rows : (n + 1) * rows]


def run_expert(xs, weights):
    return pl.pallas_call(
        functools.partial(expert_kernel, len(xs)),
        in_specs=vmem(len(xs) + 6),
        out_specs=vmem(len(xs)),
        out_shape=tuple(jax.ShapeDtypeStruct(x.shape, BF16) for x in xs),
        compiler_params=limit(),
        cost_estimate=pl.CostEstimate(flops=5_000_000_000, bytes_accessed=9_000_000, transcendentals=0),
    )(*xs, *weights)


def block_rows(at_ref, ref, per=2):
    starts = [pl.multiple_of(at_ref[b] // per * MOE_DEV, MOE_DEV) for b in range(at_ref.shape[0])]
    return jnp.concatenate([ref[pl.ds(s, MOE_DEV), :] for s in starts], 0)


def shared_far_kernel(at_ref, own_ref, other_ref, down_ref, down2_ref, low_ref, high_ref):
    total = dot(block_rows(at_ref, own_ref), down_ref[...]) + dot(block_rows(at_ref, other_ref), down2_ref[...])
    half = low_ref.shape[0]
    low_ref[...] = total[:half].astype(BF16)
    high_ref[...] = total[half:].astype(BF16)


def shared_far(blocks, own, other, down, down2):
    out = jax.ShapeDtypeStruct((blocks.shape[0] // 2 * MOE_DEV, down.shape[1]), BF16)
    return pl.pallas_call(
        shared_far_kernel,
        in_specs=[smem()] + vmem(4),
        out_specs=vmem(2),
        out_shape=(out, out),
        compiler_params=limit(),
        cost_estimate=pl.CostEstimate(flops=300_000_000, bytes_accessed=2_000_000, transcendentals=0),
    )(blocks, own, other, down, down2)


def combine_kernel(
    experts, at_ref, recv_ref, routes_ref, weight_ref, own_ref, other_ref, down_ref, down2_ref, low_ref, high_ref, *out_refs
):
    total = dot0(slot_matrix(at_ref, routes_ref, weight_ref, experts), recv_ref[...])
    total = total + dot(block_rows(at_ref, own_ref), down_ref[...]) + dot(block_rows(at_ref, other_ref), down2_ref[...])
    half = low_ref.shape[0] // MOE_DEV
    for b, out_ref in enumerate(out_refs):
        place = at_ref[b] // 4
        start = pl.multiple_of(place % half * MOE_DEV, MOE_DEV)
        near = jnp.where(place < half, low_ref[pl.ds(start, MOE_DEV), :], high_ref[pl.ds(start, MOE_DEV), :])
        out_ref[...] = (total[b * MOE_DEV : (b + 1) * MOE_DEV] + near.astype(F32)).astype(BF16)


def combine(received, routes_t, weight_t, blocks, own, other, down, down2, low, high, experts):
    width = received.shape[1]
    count = blocks.shape[0]
    return pl.pallas_call(
        functools.partial(combine_kernel, experts),
        in_specs=[smem()] + vmem(9),
        out_specs=vmem(count),
        out_shape=(jax.ShapeDtypeStruct((MOE_DEV, width), BF16),) * count,
        compiler_params=limit(),
        cost_estimate=pl.CostEstimate(flops=600_000_000, bytes_accessed=4_000_000, transcendentals=0),
    )(blocks, received, routes_t, weight_t, own, other, down, down2, low, high)


def sum_kernel(near_ref, low_ref, high_ref, out_ref):
    half = low_ref.shape[0]
    out_ref[:half] = (near_ref[:half].astype(F32) + low_ref[...].astype(F32)).astype(BF16)
    out_ref[half:] = (near_ref[half:].astype(F32) + high_ref[...].astype(F32)).astype(BF16)


def add_halves(near, low, high):
    return pl.pallas_call(
        sum_kernel,
        in_specs=vmem(3),
        out_specs=pl.BlockSpec(memory_space=pltpu.VMEM),
        out_shape=jax.ShapeDtypeStruct(near.shape, BF16),
        compiler_params=limit(),
        cost_estimate=pl.CostEstimate(flops=100_000_000, bytes_accessed=4_000_000, transcendentals=0),
    )(near, low, high)


def layer(
    q_latent,
    kv_latent,
    rope_key,
    q_gain,
    kv_gain,
    w_query,
    w_keyval,
    w_output,
    moe_input,
    moe_gain,
    routes,
    route_weight,
    expert_gate,
    expert_up,
    expert_down,
    shared_gate,
    shared_up,
    shared_down,
):
    ep = lax.axis_index("ep")
    tp = lax.axis_index("tp")
    n_ep, n_tp = lax.axis_size("ep"), lax.axis_size("tp")
    z, core = tp // 2, tp % 2
    n_z = n_tp // 2
    at = jnp.stack([ep, z, core]).astype(jnp.int32)
    swap = lambda v: lax.ppermute(v, "tp", [(i, i ^ 1) for i in range(n_tp)])
    ahead = lambda v, k: lax.ppermute(v, "tp", [(i, (i + 2 * k) % n_tp) for i in range(n_tp)])
    exchange = lambda v: lax.all_to_all(v, "ep", split_axis=0, concat_axis=0, tiled=True)
    rows = q_latent.shape[0]
    width = moe_input.shape[1]

    group = n_z // 2
    step = jnp.arange(group, dtype=jnp.int32)
    here, turned, beside = [o * 2 + core for o in ((z % 2) + 2 * step, (z + 2 * step) % n_z, 1 - z % 2 + 2 * step)]
    routes_t, weight_t = routes.T, route_weight.T

    send = dispatch(moe_input, moe_gain, routes_t, here, n_ep)
    near = exchange(send.reshape(n_ep, group * CAP, width)).reshape(n_ep * group * CAP, width)
    half_rows = near.shape[0] // 2
    far = [ahead(near[:half_rows], 1), ahead(near[half_rows:], -1)]

    gate, up, down = expert_gate[0], expert_up[0], expert_down[0]
    weights = (gate, up, swap(gate), swap(up), down, swap(down))
    shared_down2 = swap(shared_down)
    w_output2 = swap(w_output)

    positions = (ep * rows + jnp.arange(rows, dtype=jnp.int32)).astype(F32)
    half = ROPE_DIM // 2
    inverse = 10000.0 ** (-(jnp.arange(half, dtype=F32) * 2.0 / ROPE_DIM))
    angles = inverse[:, None] * positions[None, :]
    cosine, sine = jnp.cos(angles), jnp.sin(angles)
    both, kv_t = prepare(
        q_latent, q_gain, w_query.T, kv_gain, w_keyval.T, cosine, sine, kv_latent, rope_key.T
    )

    n_pair = n_ep // 2
    hand = lambda v, moves: lax.ppermute(
        v,
        ("ep", "tp"),
        [
            ((2 * s + b) * n_tp + 2 * h + r, (2 * d + r) * n_tp + 2 * h + b)
            for s, d in moves
            for b in range(2)
            for r in range(2)
            for h in range(n_z)
        ],
    )
    straight = lambda v, moves: lax.ppermute(v, "ep", [(2 * s + r, 2 * d + r) for s, d in moves for r in range(2)])
    home = [(p, p) for p in range(n_pair)]
    late = [(n_pair - 1 - p, p) for p in range(3)]
    both = hand(both, home)
    own_other = swap(both[QK:])
    q_help = straight(both[:QK], late)
    shifted = [hand(kv_t, [(p, p + k) for p in range(n_pair - k)]) for k in range(1, 5)]
    extra = [hand(kv_t, [(p, 0)]) for p in (1, 2)]
    blocks_of = lambda v: (v, swap(v))
    near_kv = blocks_of(shifted[0]) + blocks_of(shifted[1])
    far_kv = blocks_of(shifted[2]) + blocks_of(shifted[3])
    extra_kv = blocks_of(extra[0]) + blocks_of(extra[1])

    own_hidden, other_hidden = shared_hidden(at, moe_input, moe_gain, shared_gate, shared_up)
    other_hidden = swap(other_hidden)
    low, high = shared_far(beside, own_hidden, other_hidden, shared_down, shared_down2)
    low, high = ahead(low, 1), ahead(high, -1)

    state = attend(own_kernel, 4_000_000_000, at, (both, own_other), state_shapes(rows))
    state = attend(
        functools.partial(pairs_kernel, 1), 12_000_000_000, at, (both, *near_kv, *state), state_shapes(rows), stage(rows)
    )
    helped = attend(
        help_kernel, 6_000_000_000, at, (q_help, both, own_other, *near_kv, *extra_kv),
        jax.ShapeDtypeStruct((VDIM + 8, rows), F32),
        state_scratch(rows) + [pltpu.VMEM((QK, rows), BF16), pltpu.SemaphoreType.DMA],
        away=(0, 7, 8, 9, 10),
    )
    helped = straight(helped, [(p, q) for q, p in late])
    state = attend(
        functools.partial(pairs_kernel, 3), 12_000_000_000, at, (both, *far_kv, *state), state_shapes(rows), stage(rows)
    )
    heads = attend(merge_kernel, 100_000_000, at, (helped, *state), jax.ShapeDtypeStruct((VDIM, rows), BF16))

    (near_out,) = run_expert([near], weights)
    far_low, far_high = run_expert(far, weights)
    far_low, far_high = ahead(far_low, 1), ahead(far_high, -1)
    near_out = add_halves(near_out, far_low, far_high)
    returned = exchange(near_out.reshape(n_ep, group * CAP, width)).reshape(n_ep * group * CAP, width)

    sums = combine(
        returned, routes_t, weight_t, turned, own_hidden, other_hidden, shared_down, shared_down2, low, high, n_ep
    )
    parts = [sums[0]] + [ahead(sums[j], 2 * j) for j in range(1, group)]
    moe_out = functools.reduce(lambda a, b: a + b, [p.astype(F32) for p in parts]).astype(BF16)

    first = {0: heads, **{k: ahead(heads, k) for k in (1, -1, 2, -2)}}
    pieces = [first[k] for k in (0, 1, 2)] + [ahead(first[2], 1), ahead(first[2], 2), ahead(first[-2], -1)]
    pieces += [first[-2], first[-1]]
    same, cross = project_heads(at, w_output, w_output2, pieces)
    cross = lax.ppermute(
        cross,
        ("ep", "tp"),
        [
            ((2 * p + r) * n_tp + 2 * h + b, (2 * p + b) * n_tp + 2 * h + 1 - r)
            for p in range(n_pair)
            for b in range(2)
            for r in range(2)
            for h in range(n_z)
        ],
    )
    mixed = (hand(same, home).astype(F32) + cross.astype(F32)).astype(BF16)
    return (mixed, moe_out)


def solution(mesh):
    in_specs = (
        P("ep", None),
        P("ep", None),
        P("ep", None),
        P(),
        P(),
        P(None, "tp"),
        P(None, "tp"),
        P(None, "tp"),
        P("ep", None),
        P(),
        P("ep", None),
        P("ep", None),
        P("ep", None, "tp"),
        P("ep", None, "tp"),
        P("ep", "tp", None),
        P(None, "tp"),
        P(None, "tp"),
        P("tp", None),
    )
    out_specs = (P("ep", "tp"), P(("ep", "tp"), None))
    return jax.shard_map(layer, mesh=mesh, in_specs=in_specs, out_specs=out_specs, check_vma=False)
```
